32 devices in a mesh: fs: 8 (over z, x), tp: 4 (over y, core).
Axes of the slice: x: 2, y: 2, z: 4, core: 2. Of those that a mesh axis runs over, the one named last changes fastest.
Arguments:
- x_late: bfloat16 [4096, 2048], P(('fs', 'tp')), may hold values from -6 to 6
- x_early: bfloat16 [4096, 2048], P(('fs', 'tp')), may hold values from -6 to 6
- d_hidden: bfloat16 [4096, 3072], P('fs', 'tp'), may hold values from -6 to 6
- w_gate: bfloat16 [2048, 3072], P('fs', 'tp'), may hold values from -0.125 to 0.125
- w_up: bfloat16 [2048, 3072], P('fs', 'tp'), may hold values from -0.125 to 0.125
- gate_sum: float32 [2048, 3072], P('fs', 'tp'), may hold values from -192 to 192
- up_sum: float32 [2048, 3072], P('fs', 'tp'), may hold values from -192 to 192
Outputs:
- hidden_late: bfloat16 [4096, 3072], P('fs', 'tp')
- grad_input: bfloat16 [4096, 2048], P(('fs', 'tp'))
- gate_sum_out: float32 [2048, 3072], P('fs', 'tp')
- up_sum_out: float32 [2048, 3072], P('fs', 'tp')
The draws below stay inside these ranges and needn't reach their ends.
All inputs are finite; a program needn't handle non-finite values.
Results may differ from the reference program's by a relative error of at most 0.0095.
Values may be sent and summed in bfloat16 or wider, within the bound.
No kernel may reach another device: no remote copies, remote signals or barrier semaphores. Data moves between devices by JAX's collectives and lax.ppermute only.
A program may use at most 128 MiB of HBM per device.

```python
import jax
import jax.numpy as jnp
from jax import lax

D = 2048
FF = 3072
TOKENS = 4096
N_TP = 4


def with_spikes(result, rng, source, target, shards_of, factor):
    owner, partner = [(jnp.arange(result.shape[dim]) // (result.shape[dim] // shards_of)).reshape([-1 if axis == dim else 1 for axis in range(result.ndim)]) for dim in (source, target)]
    chosen = jax.random.permutation(rng, shards_of)[partner]
    strong = (owner == chosen) | (owner == (partner + shards_of // 2) % shards_of)
    return jnp.where(strong, factor * result, result)


def level_of(stream_key, extent, shards, least, largest):
    factor_of, own = 1.0, jax.random.fold_in(stream_key, 6)
    for axis_at, parts in shards:
        heights = jnp.exp(jax.random.uniform(jax.random.fold_in(own, axis_at), (parts,), jnp.float32, least / len(shards), largest / len(shards)))
        factor_of = factor_of * jnp.repeat(heights, extent[axis_at] // parts).reshape([-1 if axis == axis_at else 1 for axis in range(len(extent))])
    return factor_of


def gaussian(key, extent, spread, limit, shards=(), dtype=jnp.bfloat16):
    gain = level_of(key, extent, shards, -0.22, 0.18) if shards else 1.0
    entries = jax.random.normal(key, extent, jnp.float32) * spread * gain
    return jnp.minimum(jnp.maximum(entries, -limit), limit).astype(dtype)


def gaussian_with(own_key, dims, spread, most, cuts, heavy, held_as=jnp.bfloat16):
    entries = spread * jax.random.normal(own_key, dims, jnp.float32)
    if cuts:
        entries = entries * level_of(own_key, dims, cuts, -0.22, 0.18)
    return jnp.clip(with_spikes(entries, jax.random.fold_in(own_key, 3), *heavy), -most, most).astype(held_as)


def setup_inputs(seed: int = 0) -> dict:
    streams_of = jax.random.split(jax.random.key(seed), 8)
    return {
        "x_late": gaussian(streams_of[0], (TOKENS, D), 1.0, 6.0, ((0, 32),)),
        "x_early": gaussian_with(streams_of[1], (TOKENS, D), 1.0, 6.0, ((0, 32),), (0, 1, 32, 2.75)),
        "d_hidden": gaussian_with(streams_of[2], (TOKENS, FF), 1.0, 6.0, ((0, 8), (1, 4)), (0, 1, 8, 2.0)),
        "w_gate": gaussian(streams_of[3], (D, FF), D ** -0.5, 0.125, ((0, 8), (1, 4))),
        "w_up": gaussian(streams_of[4], (D, FF), D ** -0.5, 0.125, ((0, 8), (1, 4))),
        "gate_sum": gaussian(streams_of[5], (D, FF), (0.5 * TOKENS ** 0.5), 192.0, ((0, 8), (1, 4)), jnp.float32),
        "up_sum": gaussian(streams_of[6], (D, FF), (0.5 * TOKENS ** 0.5), 192.0, ((0, 8), (1, 4)), jnp.float32),
    }


def reference(x_late, x_early, d_hidden, w_gate, w_up, gate_sum, up_sum):
    gate_late = jnp.dot(x_late, w_gate, preferred_element_type=jnp.float32)
    up_late = jnp.dot(x_late, w_up, preferred_element_type=jnp.float32)
    sigmoid_late = jax.nn.sigmoid(gate_late)
    hidden_late = (gate_late * sigmoid_late * up_late).astype(jnp.bfloat16)
    gate_early = jnp.dot(x_early, w_gate, preferred_element_type=jnp.float32)
    up_early = jnp.dot(x_early, w_up, preferred_element_type=jnp.float32)
    sigmoid_early = jax.nn.sigmoid(gate_early)
    cotangent = d_hidden.astype(jnp.float32)
    d_gate = (cotangent * up_early * sigmoid_early * (1.0 + gate_early * (1.0 - sigmoid_early))).astype(jnp.bfloat16)
    d_up = (cotangent * gate_early * sigmoid_early).astype(jnp.bfloat16)
    span = FF // N_TP
    total = jnp.zeros((x_early.shape[0], x_early.shape[1]), jnp.float32)
    for index in range(N_TP):
        lower = index * span
        partial_value = jnp.dot(d_gate[:, lower:lower + span], w_gate[:, lower:lower + span].T, preferred_element_type=jnp.float32)
        partial_value = partial_value + jnp.dot(d_up[:, lower:lower + span], w_up[:, lower:lower + span].T, preferred_element_type=jnp.float32)
        rounded = lax.optimization_barrier(partial_value.astype(jnp.bfloat16))
        total = total + rounded.astype(jnp.float32)
    grad_input = total.astype(jnp.bfloat16)
    gate_sum_out = gate_sum + jnp.dot(x_early.T, d_gate, preferred_element_type=jnp.float32)
    up_sum_out = up_sum + jnp.dot(x_early.T, d_up, preferred_element_type=jnp.float32)
    return (hidden_late, grad_input, gate_sum_out, up_sum_out)
```

```python
import functools

import jax
import jax.numpy as jnp
from jax import lax
from jax.experimental import pallas as pl
from jax.experimental.pallas import tpu as pltpu
from jax.sharding import PartitionSpec as P


LAST = (((1,), (1,)), ((), ()))
FIRST = (((0,), (0,)), ((), ()))
BF16 = jnp.bfloat16
F32 = jnp.float32
LANES = 128
VMEM = pl.BlockSpec(memory_space=pltpu.VMEM)
ANY = pl.BlockSpec(memory_space=pl.ANY)


def derivatives(gate, up, cotangent):
    s = jax.nn.sigmoid(gate)
    d_gate = (cotangent * up * s * (1.0 + gate * (1.0 - s))).astype(BF16)
    d_up = (cotangent * gate * s).astype(BF16)
    return d_gate, d_up


def direct(x_late, x_early, d_hidden, w_gate, w_up, gate_sum, up_sum):
    rows_late = lax.all_gather(x_late, "tp", axis=0, tiled=True)
    rows_early = lax.all_gather(x_early, "tp", axis=0, tiled=True)
    full_gate = lax.all_gather(w_gate, "fs", axis=0, tiled=True)
    full_up = lax.all_gather(w_up, "fs", axis=0, tiled=True)
    gate = jnp.dot(rows_late, full_gate, preferred_element_type=F32)
    up = jnp.dot(rows_late, full_up, preferred_element_type=F32)
    hidden_late = (gate * jax.nn.sigmoid(gate) * up).astype(BF16)
    gate = jnp.dot(rows_early, full_gate, preferred_element_type=F32)
    up = jnp.dot(rows_early, full_up, preferred_element_type=F32)
    d_gate, d_up = derivatives(gate, up, d_hidden.astype(F32))
    partial = lax.dot_general(d_gate, full_gate, LAST, preferred_element_type=F32)
    partial = partial + lax.dot_general(d_up, full_up, LAST, preferred_element_type=F32)
    grad_input = lax.psum_scatter(partial.astype(BF16), "tp", scatter_dimension=0, tiled=True)
    sums = []
    for total, grad in ((gate_sum, d_gate), (up_sum, d_up)):
        grad = lax.dot_general(rows_early, grad, FIRST, preferred_element_type=F32)
        sums.append(total + lax.psum_scatter(grad, "fs", scatter_dimension=0, tiled=True))
    return (hidden_late, grad_input, *sums)


def place():
    fs, tp = lax.axis_index("fs"), lax.axis_index("tp")
    return fs // 2, lax.rem(fs, 2), tp // 2, lax.rem(tp, 2)


def call(body, outs, specs, scratch=(), flops=0):
    def run(*operands):
        moved = sum(a.size * a.dtype.itemsize for a in operands)
        moved += sum(functools.reduce(lambda p, q: p * q, s, 1) * jnp.dtype(t).itemsize for s, t in outs)
        return pl.pallas_call(
            body,
            out_shape=[jax.ShapeDtypeStruct(s, t) for s, t in outs],
            in_specs=specs,
            out_specs=[VMEM] * len(outs),
            scratch_shapes=list(scratch),
            cost_estimate=pl.CostEstimate(flops=flops, bytes_accessed=moved, transcendentals=0),
            compiler_params=pltpu.CompilerParams(vmem_limit_bytes=48 * 1024 * 1024),
        )(*operands)

    return run


def aligned(value, step=LANES):
    return pl.multiple_of(value, step)


def planned(shares):
    pair = [(i, i ^ 1) for i in range(8)]
    core = [(i, i ^ 1) for i in range(4)]
    across = [(i, i ^ 2) for i in range(4)]

    def line(*moves):
        return [(2 * a + h, 2 * b + h) for a, b in moves for h in range(2)]

    ends = line((0, 1), (1, 0), (2, 3), (3, 2))
    middle = line((1, 2), (2, 1))
    outward = line((1, 0), (2, 3))
    inward = line((0, 1), (3, 2))

    def local(x_late, x_early, d_hidden, w_gate, w_up, gate_sum, up_sum):
        rows, depth = x_early.shape
        w_rows, cols = w_gate.shape
        width = cols // 2
        tokens = 8 * rows
        plane = 2 * w_rows
        parts, start = [], 0
        for share in shares:
            size = width * share // sum(shares)
            parts.append((start, size))
            start += size

        def pack(w_gate, w_up, d_hidden, *outs):
            _, x, _, _ = place()
            mine, sent, dh_sent = outs[: len(parts)], outs[len(parts) : -1], outs[-1]
            for bit, refs in ((x, mine), (1 - x, sent)):
                for (start, size), ref in zip(parts, refs):
                    at = pl.ds(aligned(bit * width + start), size)
                    ref[:, :size] = w_gate[:, at]
                    ref[:, size:] = w_up[:, at]
            dh_sent[...] = d_hidden[:, pl.ds(aligned((1 - x) * width), width)]

        packs = [((w_rows, 2 * size), BF16) for _, size in parts]
        packed = call(pack, packs + packs + [((d_hidden.shape[0], width), BF16)], [VMEM] * 3)(
            w_gate, w_up, d_hidden
        )
        mine, sent, dh_sent = packed[: len(parts)], packed[len(parts) : -1], packed[-1]

        def plane_of(j):
            got = lax.ppermute(sent[j], "fs", pair)
            return jnp.concatenate([mine[j], got], axis=0)

        def line_of(own):
            twin = lax.ppermute(own, "fs", ends)
            inner = lax.ppermute(jnp.concatenate([own, twin], axis=0), "fs", middle)
            return own, twin, inner, lax.ppermute(inner, "fs", outward)

        def rows_of(block):
            two = jnp.concatenate([block, lax.ppermute(block, "tp", across)], axis=0)
            four = jnp.concatenate([two, lax.ppermute(two, "fs", pair)], axis=0)
            return four, lax.ppermute(four, "tp", core)

        def load_rows(low, high, held, sems):
            half = tokens // 2
            copies = []
            for t in range(4):
                source = (low, high)[t // 2].at[pl.ds(t % 2 * half // 2, half // 2)]
                copies.append(
                    pltpu.make_async_copy(source, held.at[pl.ds(t * half // 2, half // 2)], sems.at[t])
                )
                copies[-1].start()
            return copies

        def token_at(y, c, t, dy):
            dc = t // 2
            y, c = (1 - y if dy else y), (1 - c if dc else c)
            return aligned((2 * y + c) * rows)

        def early(size, start):
            def body(low, high, own, twin, inner, outer, dh, dh_got, w, d, far, near, near_twin, held, d_t, sems):
                z, x, y, c = place()
                copies = load_rows(low, high, held, sems)
                upper = z // 2
                is_inner = lax.rem(z, 2) != upper
                twin_z = jnp.where(lax.rem(z, 2) == 0, z + 1, z - 1)
                order = (z, twin_z, 2 - upper, 3 * (1 - upper))

                def at(k, dx):
                    return aligned(order[k] * plane + (1 - x if dx else x) * w_rows)

                def put(ref, k, base):
                    for dx in range(2):
                        w[pl.ds(at(k, dx), w_rows), :] = ref[base + dx * w_rows : base + (dx + 1) * w_rows, :]

                put(own, 0, 0)
                put(twin, 1, 0)

                @pl.when(is_inner)
                def _():
                    put(inner, 2, 0)
                    put(inner, 3, plane)

                @pl.when(jnp.logical_not(is_inner))
                def _():
                    put(outer, 2, 0)
                    put(outer, 3, plane)

                for t in range(4):
                    copies[t].wait()
                    two = pl.ds(t * 2 * rows, 2 * rows)
                    pre = jnp.dot(held[two, :], w[...], preferred_element_type=F32)
                    cot = []
                    for dy in range(2):
                        token = pl.ds(token_at(y, c, t, dy), rows)
                        if t % 2 == 0:
                            cot.append(dh[token, pl.ds(aligned(x * width + start), size)])
                        else:
                            cot.append(dh_got[token, pl.ds(start, size)])
                    cot = jnp.concatenate(cot, axis=0).astype(F32)
                    both = jnp.concatenate(derivatives(pre[:, :size], pre[:, size:], cot), axis=1)
                    d[two, :] = both
                    d_t[:, two] = both.T
                for k, ref in ((2, far), (3, far), (0, near), (1, near_twin)):
                    for dx in range(2):
                        base = (plane if k == 3 else 0) + dx * w_rows
                        block = jnp.dot(
                            d_t[...], held[:, pl.ds(at(k, dx), w_rows)], preferred_element_type=F32
                        )
                        ref[:, base : base + w_rows] = block.astype(ref.dtype)

            return call(
                body,
                [
                    ((depth, 2 * size), BF16),
                    ((tokens, 2 * size), BF16),
                    ((2 * size, 2 * plane), BF16),
                    ((2 * size, plane), F32),
                    ((2 * size, plane), F32),
                ],
                [ANY, ANY] + [VMEM] * 6,
                [
                    pltpu.VMEM((tokens, depth), BF16),
                    pltpu.VMEM((2 * size, tokens), BF16),
                    pltpu.SemaphoreType.DMA((4,)),
                ],
                8 * tokens * depth * size,
            )

        def late(size):
            def body(low, high, w, kept, given, held, sems):
                _, _, y, c = place()
                copies = load_rows(low, high, held, sems)
                for t in range(4):
                    copies[t].wait()
                    pre = jnp.dot(
                        held[pl.ds(t * 2 * rows, 2 * rows), :], w[...], preferred_element_type=F32
                    )
                    gate, up = pre[:, :size], pre[:, size:]
                    hidden = (gate * jax.nn.sigmoid(gate) * up).astype(BF16)
                    for dy in range(2):
                        ref = (kept, given)[t % 2]
                        ref[pl.ds(token_at(y, c, t, dy), rows), :] = hidden[dy * rows : (dy + 1) * rows]

            outs = [((tokens // 2, size), BF16)] * 2
            return call(
                body,
                outs,
                [ANY, ANY, VMEM],
                [pltpu.VMEM((tokens, depth), BF16), pltpu.SemaphoreType.DMA((4,))],
                4 * tokens * depth * size,
            )

        def input_grad(side):
            half = tokens // 2

            def body(*refs):
                d, w, out = refs[: len(parts)], refs[len(parts) : -1], refs[-1]
                for base in range(0, half, 2 * rows):
                    for at in range(0, depth, plane):
                        total = None
                        for d_j, w_j in zip(d, w):
                            term = lax.dot_general(
                                d_j[side * half + base : side * half + base + 2 * rows, :],
                                w_j[at : at + plane, :],
                                LAST,
                                preferred_element_type=F32,
                            )
                            total = term if total is None else total + term
                        out[base : base + 2 * rows, at : at + plane] = total.astype(BF16)

            return call(
                body, [((half, depth), BF16)], [VMEM] * (2 * len(parts)), (), 4 * half * depth * width
            )

        def finish(*refs):
            n = len(parts)
            gate_sum, up_sum = refs[:2]
            kept, got = refs[2 : 2 + n], refs[2 + n : 2 + 2 * n]
            gate_out, up_out = refs[-2:]
            _, x, _, _ = place()
            for bit, blocks in ((x, kept), (1 - x, got)):
                for (start, size), block in zip(parts, blocks):
                    at = pl.ds(aligned(bit * width + start), size)
                    gate_out[:, at] = gate_sum[:, at] + block[:size, :].astype(F32).T
                    up_out[:, at] = up_sum[:, at] + block[size:, :].astype(F32).T

        def join_hidden(*refs):
            n = len(parts)
            kept, got, out = refs[:n], refs[n : 2 * n], refs[-1]
            _, x, _, _ = place()
            for bit, blocks in ((x, kept), (1 - x, got)):
                for (start, size), block in zip(parts, blocks):
                    out[:, pl.ds(aligned(bit * width + start), size)] = block[...]

        lines = [line_of(plane_of(0))]
        low, high = rows_of(x_early)
        dh_got = lax.ppermute(dh_sent, "fs", pair)
        late_low, late_high = rows_of(x_late)
        full, grads, kept_sums, got_sums, kept_hidden, got_hidden = [], [], [], [], [], []
        for j, (start, size) in enumerate(parts):
            if j:
                lines.append(line_of(plane_of(j)))
            w, d, far, near, near_twin = early(size, start)(low, high, *lines[j], d_hidden, dh_got)
            full.append(w)
            grads.append(d)
            far = (far.astype(F32) + lax.ppermute(far, "fs", inward).astype(F32)).astype(BF16)
            far = lax.ppermute(far, "fs", middle).astype(F32)
            twin = lax.ppermute((near_twin + far[:, plane:]).astype(BF16), "fs", ends)
            near = near + far[:, :plane] + twin.astype(F32)
            kept_sums.append(near[:, :w_rows])
            got_sums.append(lax.ppermute(near[:, w_rows:].astype(BF16), "fs", pair))

        (away,) = input_grad(1)(*grads, *full)
        got = lax.ppermute(away, "tp", core)
        (home,) = input_grad(0)(*grads, *full)

        for j, (start, size) in enumerate(parts):
            kept, given = late(size)(late_low, late_high, full[j])
            kept_hidden.append(kept)
            got_hidden.append(lax.ppermute(given, "fs", pair))

        def add(a, b):
            return a.astype(F32) + b.astype(F32)

        def halve(array, axis, name, perm):
            keep, give = jnp.split(array, 2, axis=axis)
            return add(keep, lax.ppermute(give, name, perm))

        home = add(home, got).astype(BF16).reshape(2, 2, rows, depth)
        left, right = home[..., : depth // 2], home[..., depth // 2 :]
        left = halve(halve(left, 0, "fs", pair).astype(BF16), 1, "tp", across)
        right = halve(halve(right, 1, "tp", across).astype(BF16), 0, "fs", pair)
        grad_input = jnp.concatenate([left[0, 0], right[0, 0]], axis=1).astype(BF16)

        (hidden_late,) = call(
            join_hidden, [((tokens // 2, cols), BF16)], [VMEM] * (2 * len(parts))
        )(*kept_hidden, *got_hidden)
        gate_out, up_out = call(
            finish, [((w_rows, cols), F32)] * 2, [VMEM] * (2 + 2 * len(parts))
        )(gate_sum, up_sum, *kept_sums, *got_sums)
        return hidden_late, grad_input, gate_out, up_out

    return local


def solution(mesh):
    n_fs, n_tp = mesh.shape["fs"], mesh.shape["tp"]
    fits = (n_fs, n_tp) == (8, 4)
    return jax.shard_map(
        planned((1, 1, 1)) if fits else direct,
        mesh=mesh,
        in_specs=(
            P(("fs", "tp"), None),
            P(("fs", "tp"), None),
            P("fs", "tp"),
            P("fs", "tp"),
            P("fs", "tp"),
            P("fs", "tp"),
            P("fs", "tp"),
        ),
        out_specs=(P("fs", "tp"), P(("fs", "tp"), None), P("fs", "tp"), P("fs", "tp")),
        check_vma=False,
    )
```
